32 devices in a mesh: ep: 16 (over z, y, x), tp: 2 (over core).
Axes of the slice: x: 2, y: 2, z: 4, core: 2. Of those that a mesh axis runs over, the one named last changes fastest.
Arguments:
- tokens: bfloat16 [4096, 2048], P('ep', 'tp'), may hold values from -6 to 6
- experts: int32 [4096, 16], P('ep'), may hold values from 0 to 65535, as said below
- weights: float32 [4096, 16], P('ep'), may hold values from 0.05 to 1
- up_table: bfloat16 [65536, 2048], P('ep', 'tp'), may hold values from -0.125 to 0.125
- out_table: bfloat16 [65536, 2048], P('ep', 'tp')
- gain: float32 [2048], P('tp'), may hold values from 0.1 to 1.9
Outputs:
- normed: bfloat16 [4096, 2048], P('ep', 'tp')
The draws below stay inside these ranges and needn't reach their ends.
Inputs may be any that keep to these rules, and one draw needn't show every extreme that they name: An expert number e lies with index e // 4096 of ep. Among the rows of one index of ep, at most 512 chosen experts lie with any one index of ep, and in every draw some index of ep receives exactly 512 from every index.
All inputs are finite; a program needn't handle non-finite values.
Results may differ from the reference program's by a relative error of at most 0.006.
Values may be sent and summed in bfloat16 or wider, within the bound.
A program may use at most 128 MiB of HBM per device.

```python
import math
import jax
import jax.numpy as jnp
from jax import lax

D = 2048
SLOTS = 16
EXPERTS_PER_RANK = 4096
TOK_DEV = 256
TOKENS = 4096
EXPERTS = 65536
ROW_LIMIT = 512
N_EP = 16


def draw_experts(key, part):
    request_list = TOK_DEV * SLOTS
    slot_count = N_EP * ROW_LIMIT
    order = jax.random.permutation(jax.random.fold_in(key, 11), N_EP)
    pinned_choice = (order < N_EP // 8).astype(jnp.int32)
    slot_holder_rank = jnp.arange(slot_count, dtype=jnp.int32) // ROW_LIMIT

    def one_source(sender_rank):
        score_key = jax.random.fold_in(key, sender_rank + 100)
        random_jitter = jax.random.randint(jax.random.fold_in(score_key, 1), (slot_count,), 0, 4096, dtype=jnp.int32)
        expert_score = (pinned_choice[slot_holder_rank] * 8192 + random_jitter) * slot_count + jnp.arange(slot_count, dtype=jnp.int32)
        selected_rows = lax.top_k(expert_score, request_list)[1].astype(jnp.int32)
        owner_ranks = jax.random.permutation(jax.random.fold_in(score_key, 2), selected_rows // ROW_LIMIT)
        picked_experts = jax.random.randint(jax.random.fold_in(score_key, 3), (3, request_list), 0, EXPERTS_PER_RANK, dtype=jnp.int32)
        local = picked_experts[0] * picked_experts[1] // EXPERTS_PER_RANK * picked_experts[2] // EXPERTS_PER_RANK
        return (owner_ranks * EXPERTS_PER_RANK + local).reshape(TOK_DEV, SLOTS)
    return lax.map(one_source, jnp.arange(N_EP, dtype=jnp.int32)).reshape(TOK_DEV * N_EP, SLOTS)


def draw_out_table(key, part):
    cols = jnp.arange(D, dtype=jnp.float32) / D
    jitter = jnp.exp(jax.random.uniform(jax.random.fold_in(key, 2), (D,), jnp.float32, -0.35, 0.35))
    rowscale = jnp.exp(jax.random.uniform(jax.random.fold_in(key, 3), (EXPERTS, 1), jnp.float32, 0.0, math.log(10.0)))
    base = jax.random.normal(jax.random.fold_in(key, 6), (EXPERTS, D), jnp.float32)
    colscale = 10.0 ** cols * jitter
    return (0.1 * base * rowscale * colscale[None, :]).astype(jnp.bfloat16)


def block_scale(key, extent, cuts, least, top_value):
    level, own = 1.0, jax.random.fold_in(key, 6)
    for dim, shards_of in cuts:
        steps = jnp.exp(jax.random.uniform(jax.random.fold_in(own, dim), (shards_of,), jnp.float32, least / len(cuts), top_value / len(cuts)))
        level = level * jnp.repeat(steps, extent[dim] // shards_of).reshape([-1 if axis == dim else 1 for axis in range(len(extent))])
    return level


def scatter_about(stream_key, extent, spread, most, cuts=(), kind=jnp.bfloat16):
    level = block_scale(stream_key, extent, cuts, -0.22, 0.18) if cuts else 1.0
    values = jax.random.normal(stream_key, extent, jnp.float32) * spread * level
    return jnp.minimum(jnp.maximum(values, -most), most).astype(kind)


def setup_inputs(seed: int = 0) -> dict:
    key_of = jax.random.split(jax.random.key(seed), 7)
    tokens = scatter_about(key_of[0], (TOKENS, D), 1.0, 6.0, ((0, 16), (1, 2)))
    experts = draw_experts(jax.random.fold_in(key_of[6], 71), 0)
    weights = jnp.clip(jnp.exp(math.log(1.0) - 2.9957323 * jax.random.uniform(key_of[2], (TOKENS, SLOTS), jnp.float32) ** block_scale(key_of[2], (TOKENS, SLOTS), ((0, 16),), -0.2, 0.2)), 0.05, 1.0)
    up_table = scatter_about(key_of[3], (EXPERTS, D), D ** -0.5, 0.125, ((0, 16), (1, 2)))
    out_table = draw_out_table(jax.random.fold_in(key_of[6], 71), 0)
    gain = jnp.clip(1.0 + 0.18 * jax.random.normal(key_of[5], (D,), jnp.float32), 0.1, 1.9)
    return {"tokens": tokens, "experts": experts, "weights": weights, "up_table": up_table, "out_table": out_table, "gain": gain}


def reference(tokens, experts, weights, up_table, out_table, gain):
    blocks = tokens.shape[0] // TOK_DEV
    tok_blocks = tokens.reshape(blocks, TOK_DEV, D)
    id_blocks = experts.reshape(blocks, TOK_DEV, SLOTS)
    wt_blocks = weights.reshape(blocks, TOK_DEV, SLOTS)
    gain_f = gain.astype(jnp.float32)

    def one_block(args):
        rows, ids, wts = args
        up_rows = up_table[ids].astype(jnp.float32)
        dot = jnp.einsum('tw,tkw->tk', rows.astype(jnp.float32), up_rows)
        act = jax.nn.gelu(dot)
        contrib = (act[:, :, None] * out_table[ids].astype(jnp.float32)).astype(jnp.bfloat16)
        mixed = jnp.einsum('tk,tkw->tw', wts.astype(jnp.float32), contrib.astype(jnp.float32))
        power = lax.optimization_barrier(jnp.mean(mixed * mixed, axis=1))
        return (mixed * lax.rsqrt(power + 1e-06)[:, None] * gain_f[None, :]).astype(jnp.bfloat16)
    normed = lax.map(one_block, (tok_blocks, id_blocks, wt_blocks))
    return normed.reshape(tokens.shape[0], D)
```

```python
import functools

import jax
import jax.numpy as jnp
from jax import lax
from jax.experimental import pallas as pl
from jax.experimental.pallas import tpu as pltpu
from jax.sharding import PartitionSpec as P

LANES = 128


def owner_ranks(owner, n_ep):
    request_list = owner.shape[0]
    block_len = 512
    block_count = request_list // block_len
    onehot = (owner[:, None] == jnp.arange(n_ep, dtype=jnp.int32)[None, :]).astype(jnp.bfloat16)
    onehot_blocks = onehot.reshape(block_count, block_len, n_ep)
    row_pos = jnp.arange(block_len, dtype=jnp.int32)
    lower = (row_pos[:, None] >= row_pos[None, :]).astype(jnp.bfloat16)
    within = jnp.einsum("ij,bjn->bin", lower, onehot_blocks, preferred_element_type=jnp.float32)
    totals = within[:, block_len - 1, :]
    before = jnp.cumsum(totals, axis=0) - totals
    counted = jnp.sum((within + before[:, None, :]) * onehot_blocks.astype(jnp.float32), axis=2)
    return counted.reshape(request_list).astype(jnp.int32) - 1


def dots_kernel(rows_held, capacity, list_ref, tok_ref, up_ref, dot_ref, prod):
    sub = tok_ref.shape[1]
    base = pl.program_id(0) * capacity
    unroll = 16
    for block in range(capacity // LANES):

        def some(g, carry):
            for u in range(unroll):
                k = g * unroll + u
                word = list_ref[base + block * LANES + k]
                a = tok_ref[word // rows_held].astype(jnp.float32)
                b = up_ref[word % rows_held].astype(jnp.float32)
                prod[pl.ds(pl.multiple_of(k * sub, sub), sub), :] = a * b
            return carry

        lax.fori_loop(0, LANES // unroll, some, 0)
        if sub == 1:
            total = prod[...]
        else:
            total = prod[pl.ds(0, LANES, stride=sub), :]
            for s in range(1, sub):
                total = total + prod[pl.ds(s, LANES, stride=sub), :]
        dot_ref[0, pl.ds(block, 1), :] = jnp.sum(total.T, axis=0, keepdims=True)


def request_dots(words, tok_all, up, capacity, n_ep):
    rows_held, sub, _ = up.shape
    tok_rows = tok_all.shape[0] // n_ep
    return pl.pallas_call(
        functools.partial(dots_kernel, rows_held, capacity),
        grid_spec=pltpu.PrefetchScalarGridSpec(
            num_scalar_prefetch=1,
            grid=(n_ep,),
            in_specs=[
                pl.BlockSpec((tok_rows, sub, LANES), lambda i, w: (i, 0, 0)),
                pl.BlockSpec((rows_held, sub, LANES), lambda i, w: (0, 0, 0)),
            ],
            out_specs=pl.BlockSpec((1, capacity // LANES, LANES), lambda i, w: (i, 0, 0)),
            scratch_shapes=[pltpu.VMEM((LANES * sub, LANES), jnp.float32)],
        ),
        out_shape=jax.ShapeDtypeStruct((n_ep, capacity // LANES, LANES), jnp.float32),
        name="request_dots",
    )(words, tok_all, up)


def mix_kernel(rows_held, capacity, group, tok_rows, list_ref, coef_ref, table_ref, mix_ref, acc):
    first = pl.program_id(0) * group

    def clear(i, carry):
        acc[pl.ds(i * LANES, LANES)] = jnp.zeros((LANES,) + acc.shape[1:], acc.dtype)
        return carry

    lax.fori_loop(0, acc.shape[0] // LANES, clear, 0)

    def step(j, carry):
        places, sums = [], []
        for s in range(group):
            at = (first + s) * capacity + j
            word = list_ref[at]
            place = s * tok_rows + word // rows_held
            row = table_ref[word % rows_held].astype(jnp.float32)
            places.append(place)
            sums.append(acc[place] + coef_ref[at] * row)
        for place, total in zip(places, sums):
            acc[place] = total
        return carry

    lax.fori_loop(0, capacity, step, 0)

    def emit(i, carry):
        mix_ref[pl.ds(i * LANES, LANES)] = acc[pl.ds(i * LANES, LANES)].astype(mix_ref.dtype)
        return carry

    lax.fori_loop(0, acc.shape[0] // LANES, emit, 0)


def mix_rows(words, coef, table, capacity, n_ep, tok_rows):
    rows_held, sub, _ = table.shape
    group = 16
    return pl.pallas_call(
        functools.partial(mix_kernel, rows_held, capacity, group, tok_rows),
        grid_spec=pltpu.PrefetchScalarGridSpec(
            num_scalar_prefetch=2,
            grid=(n_ep // group,),
            in_specs=[pl.BlockSpec((rows_held, sub, LANES), lambda i, w, c: (0, 0, 0))],
            out_specs=pl.BlockSpec((group * tok_rows, sub, LANES), lambda i, w, c: (i, 0, 0)),
            scratch_shapes=[pltpu.VMEM((group * tok_rows, sub, LANES), jnp.float32)],
        ),
        out_shape=jax.ShapeDtypeStruct((n_ep * tok_rows, sub, LANES), jnp.bfloat16),
        name="mix_rows",
    )(words, coef, table)


def body(tokens, experts, weights, up_table, out_table, gain):
    n_ep = lax.axis_size("ep")
    tok_rows, width = tokens.shape
    slots = experts.shape[1]
    rows_held = up_table.shape[0]
    sub = width // LANES
    request_list = tok_rows * slots
    capacity = 2 * request_list // n_ep
    tok_all = lax.all_gather(tokens.reshape(tok_rows, sub, LANES), "ep", axis=0, tiled=True)
    flat = experts.reshape(-1)
    owner = flat // rows_held
    local_row = flat - owner * rows_held
    position = owner * capacity + owner_ranks(owner, n_ep)
    token_of = jnp.arange(request_list, dtype=jnp.int32) // slots
    send_words = (
        jnp.zeros((n_ep * capacity,), jnp.int32)
        .at[position]
        .set(token_of * rows_held + local_row, unique_indices=True)
    )
    send_weights = (
        jnp.zeros((n_ep * capacity,), jnp.float32)
        .at[position]
        .set(weights.reshape(-1), unique_indices=True)
    )
    words = lax.all_to_all(send_words.reshape(n_ep, capacity), "ep", 0, 0, tiled=True).reshape(-1)
    scales = lax.all_to_all(send_weights.reshape(n_ep, capacity), "ep", 0, 0, tiled=True)
    up = up_table.reshape(rows_held, sub, LANES)
    out = out_table.reshape(rows_held, sub, LANES)
    partial_value = request_dots(words, tok_all, up, capacity, n_ep)
    dot = lax.psum(partial_value, "tp")
    coef = (scales.reshape(dot.shape) * jax.nn.gelu(dot)).reshape(-1)
    part = mix_rows(words, coef, out, capacity, n_ep, tok_rows)
    mixed = lax.psum_scatter(part, "ep", scatter_dimension=0, tiled=True).astype(jnp.float32)
    square = lax.psum(jnp.sum(mixed * mixed, axis=(1, 2)), "tp")
    scale = lax.rsqrt(square / (width * lax.axis_size("tp")) + 1e-06)
    normed = mixed * scale[:, None, None] * gain.reshape(1, sub, LANES)
    return normed.astype(jnp.bfloat16).reshape(tok_rows, width)


def solution(mesh):
    placed = (P("ep", "tp"), P("ep", None), P("ep", None), P("ep", "tp"), P("ep", "tp"), P("tp"))
    return jax.shard_map(body, mesh=mesh, in_specs=placed, out_specs=P("ep", "tp"), check_vma=False)
```

```python
import functools
import math

import jax
import jax.numpy as jnp
from jax import lax
from jax.experimental import pallas as pl
from jax.experimental.pallas import tpu as pltpu
from jax.sharding import PartitionSpec as P

LANES = 128


def owner_ranks(owner, n_ep):
    request_list = owner.shape[0]
    block_len = 512
    block_count = request_list // block_len
    onehot = (owner[:, None] == jnp.arange(n_ep, dtype=jnp.int32)[None, :]).astype(jnp.bfloat16)
    onehot_blocks = onehot.reshape(block_count, block_len, n_ep)
    row_pos = jnp.arange(block_len, dtype=jnp.int32)
    lower = (row_pos[:, None] >= row_pos[None, :]).astype(jnp.bfloat16)
    within = jnp.einsum("ij,bjn->bin", lower, onehot_blocks, preferred_element_type=jnp.float32)
    totals = within[:, block_len - 1, :]
    before = jnp.cumsum(totals, axis=0) - totals
    counted = jnp.sum((within + before[:, None, :]) * onehot_blocks.astype(jnp.float32), axis=2)
    return counted.reshape(request_list).astype(jnp.int32) - 1


def dots_kernel(capacity, place_ref, row_ref, tok_ref, up_ref, dot_ref, prod):
    sub = tok_ref.shape[1]
    base = pl.program_id(0) * capacity
    unroll = 32
    for block in range(capacity // LANES):

        def some(g, carry):
            for u in range(unroll):
                k = g * unroll + u
                at = base + block * LANES + k
                a = tok_ref[place_ref[at]].astype(jnp.float32)
                b = up_ref[row_ref[at]].astype(jnp.float32)
                prod[pl.ds(pl.multiple_of(k * sub, sub), sub), :] = a * b
            return carry

        lax.fori_loop(0, LANES // unroll, some, 0)
        if sub == 1:
            total = prod[...]
        else:
            total = prod[pl.ds(0, LANES, stride=sub), :]
            for s in range(1, sub):
                total = total + prod[pl.ds(s, LANES, stride=sub), :]
        dot_ref[0, pl.ds(block, 1), :] = jnp.sum(total.T, axis=0, keepdims=True)


def request_dots(places, rows, tok_all, up, capacity, n_ep):
    rows_held, sub, _ = up.shape
    tok_rows = tok_all.shape[0] // n_ep
    return pl.pallas_call(
        functools.partial(dots_kernel, capacity),
        grid_spec=pltpu.PrefetchScalarGridSpec(
            num_scalar_prefetch=2,
            grid=(n_ep,),
            in_specs=[
                pl.BlockSpec((tok_rows, sub, LANES), lambda i, p, r: (i, 0, 0)),
                pl.BlockSpec((rows_held, sub, LANES), lambda i, p, r: (0, 0, 0)),
            ],
            out_specs=pl.BlockSpec((1, capacity // LANES, LANES), lambda i, p, r: (i, 0, 0)),
            scratch_shapes=[pltpu.VMEM((LANES * sub, LANES), jnp.float32)],
        ),
        out_shape=jax.ShapeDtypeStruct((n_ep, capacity // LANES, LANES), jnp.float32),
        name="request_dots",
    )(places, rows, tok_all, up)


def mix_kernel(capacity, group, place_ref, row_ref, coef_ref, table_ref, mix_ref, acc):
    first = pl.program_id(0) * group

    def clear(i, carry):
        acc[pl.ds(i * LANES, LANES)] = jnp.zeros((LANES,) + acc.shape[1:], acc.dtype)
        return carry

    lax.fori_loop(0, acc.shape[0] // LANES, clear, 0)

    def step(j, carry):
        places, sums = [], []
        for s in range(group):
            at = (first + s) * capacity + j
            place = place_ref[at]
            row = table_ref[row_ref[at]].astype(jnp.float32)
            places.append(place)
            sums.append(acc[place] + coef_ref[at] * row)
        for place, total in zip(places, sums):
            acc[place] = total
        return carry

    lax.fori_loop(0, capacity, step, 0)

    def emit(i, carry):
        mix_ref[pl.ds(i * LANES, LANES)] = acc[pl.ds(i * LANES, LANES)].astype(mix_ref.dtype)
        return carry

    lax.fori_loop(0, acc.shape[0] // LANES, emit, 0)


def mix_rows(places, rows, coef, table, capacity, n_ep, tok_rows, group):
    rows_held, sub, _ = table.shape
    return pl.pallas_call(
        functools.partial(mix_kernel, capacity, group),
        grid_spec=pltpu.PrefetchScalarGridSpec(
            num_scalar_prefetch=3,
            grid=(n_ep // group,),
            in_specs=[pl.BlockSpec((rows_held, sub, LANES), lambda i, p, r, c: (0, 0, 0))],
            out_specs=pl.BlockSpec((group * tok_rows, sub, LANES), lambda i, p, r, c: (i, 0, 0)),
            scratch_shapes=[pltpu.VMEM((group * tok_rows, sub, LANES), jnp.float32)],
        ),
        out_shape=jax.ShapeDtypeStruct((n_ep * tok_rows, sub, LANES), jnp.bfloat16),
        name="mix_rows",
    )(places, rows, coef, table)


def body(tokens, experts, weights, up_table, out_table, gain):
    n_ep = lax.axis_size("ep")
    tok_rows, width = tokens.shape
    slots = experts.shape[1]
    rows_held = up_table.shape[0]
    sub = width // LANES
    request_list = tok_rows * slots
    capacity = 2 * request_list // n_ep
    tok_all = lax.all_gather(tokens.reshape(tok_rows, sub, LANES), "ep", axis=0, tiled=True)
    flat = experts.reshape(-1)
    owner = flat // rows_held
    local_row = flat - owner * rows_held
    position = owner * capacity + owner_ranks(owner, n_ep)
    token_of = jnp.arange(request_list, dtype=jnp.int32) // slots
    send_words = (
        jnp.zeros((n_ep * capacity,), jnp.int32)
        .at[position]
        .set(token_of * rows_held + local_row, unique_indices=True)
    )
    send_weights = (
        jnp.zeros((n_ep * capacity,), jnp.float32)
        .at[position]
        .set(weights.reshape(-1), unique_indices=True)
    )
    words = lax.all_to_all(send_words.reshape(n_ep, capacity), "ep", 0, 0, tiled=True)
    token_at = words // rows_held
    row_at = (words % rows_held).reshape(-1)
    group = math.gcd(n_ep, 16)
    first = (jnp.arange(n_ep, dtype=jnp.int32) % group) * tok_rows
    place_at = (token_at + first[:, None]).reshape(-1)
    scales = lax.all_to_all(send_weights.reshape(n_ep, capacity), "ep", 0, 0, tiled=True)
    up = up_table.reshape(rows_held, sub, LANES)
    out = out_table.reshape(rows_held, sub, LANES)
    partial_value = request_dots(token_at.reshape(-1), row_at, tok_all, up, capacity, n_ep)
    dot = lax.psum(partial_value, "tp")
    coef = (scales.reshape(dot.shape) * jax.nn.gelu(dot)).reshape(-1)
    part = mix_rows(place_at, row_at, coef, out, capacity, n_ep, tok_rows, group)
    mixed = lax.psum_scatter(part, "ep", scatter_dimension=0, tiled=True).astype(jnp.float32)
    square = lax.psum(jnp.sum(mixed * mixed, axis=(1, 2)), "tp")
    scale = lax.rsqrt(square / (width * lax.axis_size("tp")) + 1e-06)
    normed = mixed * scale[:, None, None] * gain.reshape(1, sub, LANES)
    return normed.astype(jnp.bfloat16).reshape(tok_rows, width)


def solution(mesh):
    placed = (P("ep", "tp"), P("ep", None), P("ep", None), P("ep", "tp"), P("ep", "tp"), P("tp"))
    return jax.shard_map(body, mesh=mesh, in_specs=placed, out_specs=P("ep", "tp"), check_vma=False)
```
